512 devices in a mesh: rep: 2 (over z_hi), fs: 32 (over z_lo, y), tp: 8 (over x, core).
Axes of the slice: x: 4, y: 8, z: 8 (z_hi: 2, z_lo: 4; z = z_hi * 4 + z_lo), core: 2. Of those that a mesh axis runs over, the one named last changes fastest.
Arguments:
- x_later: bfloat16 [8192, 2048], P(('rep', 'fs')), may hold values from -6 to 6
- kept_input_rows: bfloat16 [8192, 2048], P(('rep', 'fs')), may hold values from -6 to 6
- cotangent: bfloat16 [8192, 2048], P(('rep', 'fs')), may hold values from -8 to 8
- norm_gain_vector: float32 [2048], replicated, may hold values from 0.1 to 1.9
- up_weight: bfloat16 [2048, 4096], P('fs', 'tp'), may hold values from -0.125 to 0.125
- down_weight: bfloat16 [4096, 2048], P('tp', 'fs'), may hold values from -0.09375 to 0.09375
- up_sum: float32 [2048, 4096], P('fs', 'tp'), may hold values from -6 to 6
- down_sum: float32 [4096, 2048], P('tp', 'fs'), may hold values from -6 to 6
Outputs:
- mixed: bfloat16 [8192, 2048], P(('rep', 'fs'))
- input_gradient_rows: bfloat16 [8192, 2048], P(('rep', 'fs'))
- up_total: float32 [2048, 4096], P('fs', 'tp')
- down_total: float32 [4096, 2048], P('tp', 'fs')
The draws below stay inside these ranges and needn't reach their ends.
All inputs are finite; a program needn't handle non-finite values.
Results may differ from the reference program's by a relative error of at most 0.018.
Values may be sent and summed in bfloat16 or wider, within the bound.
No kernel may reach another device: no remote copies, remote signals or barrier semaphores. Data moves between devices by JAX's collectives and lax.ppermute only.
A program may use at most 64 MiB of HBM per device.

```python
import jax
import jax.numpy as jnp
from jax import lax

D = 2048
FF = 4096
TOKENS = 8192
N_TP = 8


def with_spikes(values, own_key, source, target, shards_of, factor):
    def block_of(dim):
        return (jnp.arange(values.shape[dim]) // (values.shape[dim] // shards_of)).reshape((-1,) + (1,) * (values.ndim - 1 - dim))

    one_side = jax.random.permutation(own_key, shards_of)[block_of(target)]
    far = (block_of(target) + shards_of // 2) % shards_of
    return jnp.where((block_of(source) == one_side) | (block_of(source) == far), factor * values, values)


def block_scale(stream_key, extent, cuts, least, top_value):
    gain, own = 1.0, jax.random.fold_in(stream_key, 6)
    for position, blocks in cuts:
        draws = jnp.exp(jax.random.uniform(jax.random.fold_in(own, position), (blocks,), jnp.float32, least / len(cuts), top_value / len(cuts)))
        gain = gain * jnp.repeat(draws, extent[position] // blocks).reshape([-1 if axis == position else 1 for axis in range(len(extent))])
    return gain


def bell_draw(key, shape, scale, most, cuts=(), kind=jnp.bfloat16):
    entries = scale * jax.random.normal(key, shape, jnp.float32)
    if cuts:
        entries = entries * block_scale(key, shape, cuts, -0.22, 0.18)
    return jnp.clip(entries, -most, most).astype(kind)


def gaussian_with(stream_key, dims, scale, limit, pieces, heavy, held_as=jnp.bfloat16):
    entries = scale * jax.random.normal(stream_key, dims, jnp.float32)
    if pieces:
        entries = entries * block_scale(stream_key, dims, pieces, -0.22, 0.18)
    return jnp.clip(with_spikes(entries, jax.random.fold_in(stream_key, 3), *heavy), -limit, limit).astype(held_as)


def setup_inputs(seed: int = 0) -> dict:
    key_list = jax.random.split(jax.random.key(seed), 9)
    return {
        "x_later": bell_draw(key_list[0], (TOKENS, D), 1.0, 6.0, ((0, 64),)),
        "kept_input_rows": bell_draw(key_list[1], (TOKENS, D), 1.0, 6.0, ((0, 64),)),
        "cotangent": gaussian_with(key_list[2], (TOKENS, D), 1.0, 8.0, ((0, 64),), (0, 1, 64, 4.0)),
        "norm_gain_vector": jnp.clip(1.0 + 0.18 * jax.random.normal(key_list[3], (D,), jnp.float32), 0.1, 1.9),
        "up_weight": bell_draw(key_list[4], (D, FF), D ** -0.5, 0.125, ((0, 32), (1, 8))),
        "down_weight": bell_draw(key_list[5], (FF, D), FF ** -0.5, 0.09375, ((0, 8), (1, 32))),
        "up_sum": bell_draw(key_list[6], (D, FF), 1.0, 6.0, ((0, 32), (1, 8)), jnp.float32),
        "down_sum": bell_draw(key_list[7], (FF, D), 1.0, 6.0, ((0, 8), (1, 32)), jnp.float32),
    }


EPSILON = 1e-06

def norm_partial_terms(values, norm_gain_vector):
    floats = values.astype(jnp.float32)
    inverse = lax.rsqrt(lax.optimization_barrier(jnp.mean(floats * floats, axis=-1, keepdims=True)) + EPSILON)
    unit_rows = floats * inverse
    normed = (unit_rows * norm_gain_vector).astype(jnp.bfloat16)
    return (inverse, unit_rows, normed)

def block_sum(left, right_weight, transpose_right):
    width = FF // N_TP
    result = jnp.zeros((left.shape[0], D), jnp.float32)
    for block in range(N_TP):
        left_block = left[:, block * width:(block + 1) * width]
        if transpose_right:
            part = jnp.dot(left_block, right_weight[:, block * width:(block + 1) * width].T, preferred_element_type=jnp.float32)
        else:
            part = jnp.dot(left_block, right_weight[block * width:(block + 1) * width], preferred_element_type=jnp.float32)
        rounded = lax.optimization_barrier(part.astype(jnp.bfloat16))
        result = result + rounded.astype(jnp.float32)
    return result

def reference(x_later, kept_input_rows, cotangent, norm_gain_vector, up_weight, down_weight, up_sum, down_sum):
    inv_later, unit_later, normed_later = norm_partial_terms(x_later, norm_gain_vector)
    inverse_rms_kept, unit_kept_rows, normed_kept_rows = norm_partial_terms(kept_input_rows, norm_gain_vector)
    pre_later = jnp.dot(normed_later, up_weight, preferred_element_type=jnp.float32)
    pre_saved = jnp.dot(normed_kept_rows, up_weight, preferred_element_type=jnp.float32)
    hidden_later = jnp.square(jax.nn.relu(pre_later)).astype(jnp.bfloat16)
    hidden_saved = jnp.square(jax.nn.relu(pre_saved)).astype(jnp.bfloat16)
    mixed = block_sum(hidden_later, down_weight, False).astype(jnp.bfloat16)
    hidden_grad = jnp.dot(cotangent, down_weight.T, preferred_element_type=jnp.float32)
    pre_grad = (hidden_grad * 2.0 * jax.nn.relu(pre_saved)).astype(jnp.bfloat16)
    normed_grad = block_sum(pre_grad, up_weight, True)
    scaled_rows = normed_grad * norm_gain_vector
    input_gradient_rows = (inverse_rms_kept * (scaled_rows - unit_kept_rows * lax.optimization_barrier(jnp.mean(scaled_rows * unit_kept_rows, axis=-1, keepdims=True)))).astype(jnp.bfloat16)
    grad_scale = TOKENS ** (-0.5)
    up_total = up_sum + grad_scale * jnp.dot(normed_kept_rows.T, pre_grad, preferred_element_type=jnp.float32)
    down_total = down_sum + grad_scale * jnp.dot(hidden_saved.T, cotangent, preferred_element_type=jnp.float32)
    return (mixed, input_gradient_rows, up_total, down_total)
```

```python
import jax
import jax.numpy as jnp
from jax import lax
from jax.sharding import Mesh
from jax.sharding import PartitionSpec as P

FS = ("zl", "yh", "yl")
Y = ("yh", "yl")
Z = ("rep", "zl")
TP = ("x", "core")
ROWS = ("rep", "zl", "yh", "yl")

EPSILON = 1e-06
F32 = jnp.float32
BF16 = jnp.bfloat16
CONTRACT_LAST = (((1,), (1,)), ((), ()))
CONTRACT_FIRST = (((0,), (0,)), ((), ()))


def around(values, axes, step):
    count = lax.axis_size(axes)
    return lax.ppermute(values, axes, [(i, (i + step) % count) for i in range(count)])


def swapped(values, axis):
    return lax.ppermute(values, axis, [(0, 1), (1, 0)])


def exchanged(blocks, axes):
    return lax.all_to_all(blocks, axes, split_axis=0, concat_axis=0, tiled=True)


def norm_terms(values, gain):
    floats = values.astype(F32)
    inverse = lax.rsqrt(jnp.mean(floats * floats, axis=-1, keepdims=True) + EPSILON)
    unit = floats * inverse
    return inverse, unit, (unit * gain).astype(BF16)


def body(x_later, kept, cotangent, gain, up_weight, down_weight, up_sum, down_sum):
    rows, width = x_later.shape
    half = rows // 2
    depth, units = up_weight.shape
    own_units = units // 2
    n_y = lax.axis_size(Y)
    n_z = lax.axis_size("zl")
    n_x = lax.axis_size("x")
    grad_scale = float(rows * lax.axis_size("rep") * lax.axis_size(FS)) ** (-0.5)
    core = lax.axis_index("core")
    pair = lax.axis_index("yl")
    z = lax.axis_index("zl")

    both = jnp.stack([up_weight, down_weight.T])
    halves = both.reshape(2, depth, 2, own_units).transpose(2, 0, 1, 3)
    copies = jnp.broadcast_to(halves[None], (n_y // 2, *halves.shape)).reshape(n_y, 2, depth, own_units)
    held = exchanged(copies, Y)

    def split_rows(a):
        mine = lax.dynamic_slice_in_dim(a, core * half, half, 0)
        other = lax.dynamic_slice_in_dim(a, (1 - core) * half, half, 0)
        return mine, other

    own = [split_rows(a) for a in (kept, x_later, cotangent)]
    partner_mine = swapped(jnp.stack([mine for mine, _ in own]), "yl")

    w_next = around(held, Z, 1)
    w_prev = around(held, Z, -1)
    w_far_low = around(held[: n_y // 2], Z, 2)
    w_far_high = around(held[n_y // 2 :], Z, -2)

    partner_other = swapped(partner_mine, "core")
    kept_rows, later_rows, cot_rows = (
        jnp.concatenate([own[i][0], own[i][1], partner_mine[i], partner_other[i]], axis=0)
        for i in range(3)
    )
    inverse, unit, normed_saved = norm_terms(kept_rows, gain)
    _, _, normed_later = norm_terms(later_rows, gain)

    weights = jnp.zeros((2, n_z, n_y, depth, own_units), BF16)

    def placed(weights, piece, at, first=0):
        block = piece.transpose(1, 0, 2, 3)[:, None]
        return lax.dynamic_update_slice(weights, block, (0, lax.rem(at, n_z), first, 0, 0))

    weights = placed(weights, held, z)
    weights = placed(weights, w_next, z + n_z - 1)
    weights = placed(weights, w_prev, z + 1)
    weights = placed(weights, w_far_low, z + 2)
    weights = placed(weights, w_far_high, z + 2, n_y // 2)
    up_all = weights[0].reshape(width, own_units)
    down_all = weights[1].reshape(width, own_units)

    pre = jnp.dot(
        jnp.concatenate([normed_saved, normed_later]), up_all, preferred_element_type=F32
    )
    pre_saved = jax.nn.relu(pre[: 2 * rows])
    pre_later = jax.nn.relu(pre[2 * rows :])
    hidden_saved = jnp.square(pre_saved).astype(BF16)
    hidden_later = jnp.square(pre_later).astype(BF16)
    hidden_grad = jnp.dot(cot_rows, down_all, preferred_element_type=F32)
    pre_grad = (hidden_grad * 2.0 * pre_saved).astype(BF16)

    up_part = lax.dot_general(normed_saved, pre_grad, CONTRACT_FIRST, preferred_element_type=F32)
    down_part = lax.dot_general(cot_rows, hidden_saved, CONTRACT_FIRST, preferred_element_type=F32)
    parts = jnp.stack([up_part, down_part]).reshape(2, n_z, n_y, depth, own_units)

    def block_of(at):
        return lax.dynamic_index_in_dim(parts, lax.rem(at, n_z), 1, keepdims=False)

    far = block_of(z + 2).astype(BF16)
    g_next = around(block_of(z + 1).astype(BF16), Z, 1)
    g_prev = around(block_of(z + n_z - 1).astype(BF16), Z, -1)
    g_far_low = around(far[:, : n_y // 2], Z, 2)
    g_far_high = around(far[:, n_y // 2 :], Z, -2)

    mixed_part = lax.dot_general(hidden_later, down_all, CONTRACT_LAST, preferred_element_type=F32)
    back_part = lax.dot_general(pre_grad, up_all, CONTRACT_LAST, preferred_element_type=F32)
    outs = jnp.stack([mixed_part, back_part]).reshape(2, 2, 2, half, width)
    from_core = swapped(outs[:, :, 1].astype(BF16), "core")
    core_sum = outs[:, :, 0] + from_core.astype(F32)
    first = jnp.where(pair == 0, core_sum[:, 0], core_sum[:, 1])
    second = jnp.where(pair == 0, core_sum[:, 1], core_sum[:, 0])
    columns = width // n_x
    sends = jnp.stack([first, second]).astype(BF16).reshape(2, 2, half, n_x, columns)
    sends = sends.transpose(0, 3, 1, 2, 4).reshape(2 * n_x, 2, half, columns)
    summed = exchanged(sends, ("yl", "x")).astype(F32).sum(axis=0).astype(BF16)

    block = block_of(z)
    far_sum = jnp.concatenate([g_far_low, g_far_high], axis=1)
    block = block + g_next.astype(F32) + g_prev.astype(F32) + far_sum.astype(F32)
    over_y = exchanged(block.astype(BF16).transpose(1, 0, 2, 3), Y).astype(F32)
    shard = over_y.reshape(n_y // 2, 2, 2, depth, own_units).sum(axis=0)
    shard = (shard * grad_scale).astype(BF16)
    other_rep = swapped(shard, "rep")

    gathered = exchanged(jnp.broadcast_to(summed[None], (n_x, *summed.shape)), "x")
    gathered = gathered.transpose(1, 2, 0, 3).reshape(2, half, width)
    scaled = gathered[1].astype(F32) * gain
    unit_mine = unit[:half]
    input_grad = inverse[:half] * (
        scaled - unit_mine * jnp.mean(scaled * unit_mine, axis=-1, keepdims=True)
    )
    mine = jnp.stack([gathered[0], input_grad.astype(BF16)])
    theirs = swapped(mine, "core")
    mixed, input_gradient_rows = (
        jnp.concatenate(
            [jnp.where(core == 0, mine[i], theirs[i]), jnp.where(core == 0, theirs[i], mine[i])]
        )
        for i in range(2)
    )

    total = (shard.astype(F32) + other_rep.astype(F32)).transpose(1, 2, 0, 3)
    total = total.reshape(2, depth, units)
    return mixed, input_gradient_rows, up_sum + total[0], down_sum + total[1].T


def solution(mesh):
    finer = Mesh(
        mesh.devices.reshape(mesh.shape["rep"], 4, 4, 2, 4, 2),
        ("rep", "zl", "yh", "yl", "x", "core"),
    )
    return jax.shard_map(
        body,
        mesh=finer,
        in_specs=(
            P(ROWS, None),
            P(ROWS, None),
            P(ROWS, None),
            P(),
            P(FS, TP),
            P(TP, FS),
            P(FS, TP),
            P(TP, FS),
        ),
        out_specs=(P(ROWS, None), P(ROWS, None), P(FS, TP), P(TP, FS)),
        check_vma=False,
    )
```
